32 devices in a mesh: gr: 2 (over x), fs: 8 (over z, y), tp: 2 (over core).
Axes of the slice: x: 2, y: 2, z: 4, core: 2. Of those that a mesh axis runs over, the one named last changes fastest.
Arguments:
- tokens: bfloat16 [6144, 2048], P(('gr', 'fs')), may hold values from -6 to 6
- routes: int32 [6144, 4], P(('gr', 'fs')), may hold values from 0 to 7, all different within a row; in each aligned block of 384 rows (0 to 383, 384 to 767, ...) at most 288 rows name the same one
- route_scores: float32 [6144, 4], P(('gr', 'fs')), may hold values from -6 to 6
- norm_gain: float32 [2048], P(('gr', 'fs')), may hold values from 0.1 to 1.9
- gate_master: float32 [8, 2048, 1024], P(None, ('gr', 'fs'), 'tp'), may hold values from -0.875 to 0.875
- up_master: float32 [8, 2048, 1024], P(None, ('gr', 'fs'), 'tp'), may hold values from -0.875 to 0.875
- down_master: float32 [8, 1024, 2048], P(None, ('gr', 'fs'), 'tp'), may hold values from -0.1875 to 0.1875
Outputs:
- gate_weights: bfloat16 [8, 2048, 1024], P('fs', None, 'tp')
- up_weights: bfloat16 [8, 2048, 1024], P('fs', None, 'tp')
- down_weights: bfloat16 [8, 1024, 2048], P('fs', None, 'tp')
- mixed: bfloat16 [6144, 2048], P(('gr', 'fs'), 'tp')
The draws below stay inside these ranges and needn't reach their ends.
Inputs may be any that keep to these rules, and one draw needn't show every extreme that they name: `routes`: each row names 4 different experts; among the rows of one index of gr+fs no expert is named more than 288 times, a bound that some block reaches.
All inputs are finite; a program needn't handle non-finite values.
Results may differ from the reference program's by a relative error of at most 0.0085.
Values may be sent and summed in bfloat16 or wider, within the bound.
A program may use at most 128 MiB of HBM per device.

```python
import math
import jax
import jax.numpy as jnp
import numpy as np
from jax import lax

D = 2048
FF = 1024
TOP = 4
TOK_DEV = 384
EXPERTS = 8
CAP = 288
TOKENS = 6144
N_GR = 2
N_FS = 8


def block_scale(rng, dims, shards, low, largest):
    def one(dim, blocks):
        draws = jax.random.uniform(jax.random.fold_in(jax.random.fold_in(rng, 6), dim), (blocks,), jnp.float32, low / len(shards), largest / len(shards))
        return jnp.repeat(jnp.exp(draws), dims[dim] // blocks).reshape((-1,) + (1,) * (len(dims) - dim - 1))

    loudness = one(*shards[0])
    for cut in shards[1:]:
        loudness = loudness * one(*cut)
    return loudness


def assign_block(key, own, number, rows, number_of, top, most, lean):
    ranking = jax.random.permutation(key, number_of)
    crowded, usual = shares(number_of, rows * top, most, lean, True), shares(number_of, rows * top, most, lean, False)
    places = jnp.arange(number_of)

    def named(lengths, turn):
        used = int((lengths > 0).sum())
        fixed = max(1, used // 4)
        moved = fixed + (places - fixed + turn * (used - fixed)) % max(1, number_of - fixed)
        return jnp.zeros((number_of,), jnp.int32).at[ranking[jnp.where(places < fixed, places, moved)]].set(jnp.asarray(lengths, jnp.int32))

    lengths = jnp.where(number % 4 == 0, named(crowded, number // 4), named(usual, number - number // 4 - 1))
    mixed = jax.random.permutation(jax.random.fold_in(own, 3), number_of)
    donor, taker = mixed[0:number_of // 2 * 2:2], mixed[1:number_of // 2 * 2:2]
    slack = jnp.minimum(lengths[donor] - 1, most - lengths[taker]) // 2
    slack = jnp.where((donor == ranking[0]) | (taker == ranking[0]) | (lengths[taker] == 0), 0, jnp.maximum(slack, 0))
    moved = jax.random.randint(jax.random.fold_in(own, 4), (number_of // 2,), 0, 1 << 20) % (slack + 1)
    lengths = lengths.at[donor].add(-moved).at[taker].add(moved)
    members = jnp.searchsorted(jnp.cumsum(lengths), jnp.arange(rows * top), side="right").astype(jnp.int32)
    grid = members.reshape(top, rows).T
    grid = grid[jax.random.permutation(jax.random.fold_in(own, 1), rows)]
    turn = jax.random.randint(jax.random.fold_in(own, 2), (rows, 1), 0, top)
    return jnp.take_along_axis(grid, (jnp.arange(top)[None, :] + turn) % top, axis=1)


def shares(count, total, most, slope, full):
    portions = [(1 << 20) // math.isqrt(standing ** slope) + 1 for standing in range(1, count + 1)]
    largest = most if full else min(most, max(-(-total // count), total * portions[0] // sum(portions)))
    least = 1 if total - largest >= count - 1 else 0
    holding, spare = [largest] + [least] * (count - 1), total - largest - least * (count - 1)
    while spare > 0:
        movable = [i for i in range(1, count) if holding[i] < largest] or [i for i in range(1, count) if holding[i] < most]
        whole, remaining = sum([portions[i] for i in movable]), spare
        for i in movable:
            extra = min(most - holding[i], max(1, remaining * portions[i] // whole), spare)
            holding[i] = holding[i] + extra
            spare = spare - extra
    return np.array(holding)


def bell_draw(own_key, dims, scale, bound, pieces=(), kind=jnp.bfloat16):
    loudness = block_scale(own_key, dims, pieces, -0.22, 0.18) if pieces else 1.0
    values = jax.random.normal(own_key, dims, jnp.float32) * scale * loudness
    return jnp.minimum(jnp.maximum(values, -bound), bound).astype(kind)


def setup_inputs(seed: int = 0) -> dict:
    keys = jax.random.split(jax.random.key(seed), 8)
    tokens = bell_draw(keys[0], (TOKENS, D), 1.0, 6.0, ((0, 16),))
    routes_keys = jax.random.split(jax.random.fold_in(keys[1], 1), TOKENS // TOK_DEV)
    routes_turns = jax.random.permutation(jax.random.fold_in(keys[1], 3), TOKENS // TOK_DEV)
    routes = jax.vmap(lambda own, number: assign_block(jax.random.fold_in(keys[1], 2), own, number, TOK_DEV, EXPERTS, TOP, CAP, 1))(routes_keys, routes_turns).reshape((TOKENS, TOP))
    route_scores = bell_draw(keys[2], (TOKENS, TOP), 1.0, 6.0, ((0, 16),), jnp.float32)
    norm_gain = jnp.clip(1.0 + 0.18 * jax.random.normal(keys[3], (D,), jnp.float32), 0.1, 1.9)
    gate_master = bell_draw(keys[4], (EXPERTS, D, FF), 0.055, 0.875, ((1, 16), (2, 2)), jnp.float32)
    up_master = bell_draw(keys[5], (EXPERTS, D, FF), 0.055, 0.875, ((1, 16), (2, 2)), jnp.float32)
    down_master = bell_draw(keys[6], (EXPERTS, FF, D), FF ** -0.5, 0.1875, ((1, 16), (2, 2)), jnp.float32)
    return dict(tokens=tokens, routes=routes, route_scores=route_scores, norm_gain=norm_gain, gate_master=gate_master, up_master=up_master, down_master=down_master)


NORM_EPS = 1e-05
CLAMP_LIMIT = 7.0
GLU_ALPHA = 1.702

def normalize(tokens):
    values = tokens.astype(jnp.float32)
    centre = lax.optimization_barrier(jnp.mean(values, -1, keepdims=True))
    spread = lax.optimization_barrier(jnp.mean(jnp.square(values - centre), -1, keepdims=True))
    return ((values - centre) * lax.rsqrt(spread + NORM_EPS)).astype(jnp.bfloat16)

def reference(tokens, routes, route_scores, norm_gain, gate_master, up_master, down_master):
    gate_weights = (norm_gain[None, :, None] * gate_master).astype(jnp.bfloat16)
    up_weights = (norm_gain[None, :, None] * up_master).astype(jnp.bfloat16)
    down_weights = down_master.astype(jnp.bfloat16)
    normed = normalize(tokens)
    padded = jnp.concatenate([normed, jnp.zeros((1, D), jnp.bfloat16)], axis=0)
    chosen = routes.reshape(-1)
    assigned = chosen.shape[0]
    mixing = jax.nn.softmax(route_scores.astype(jnp.float32), axis=-1).reshape(-1)
    mixing = jnp.concatenate([mixing, jnp.zeros((1,), jnp.float32)], axis=0)
    most = N_GR * N_FS * CAP

    def one_expert(total, expert):
        picked = jnp.nonzero(chosen == expert, size=most, fill_value=assigned)[0].astype(jnp.int32)
        token_rows = (picked // TOP).astype(jnp.int32)
        rows = padded[token_rows]
        w_gate = lax.dynamic_index_in_dim(gate_weights, expert, 0, keepdims=False)
        w_up = lax.dynamic_index_in_dim(up_weights, expert, 0, keepdims=False)
        w_down = lax.dynamic_index_in_dim(down_weights, expert, 0, keepdims=False)
        gate_pre = jnp.minimum(jnp.dot(rows, w_gate, preferred_element_type=jnp.float32), CLAMP_LIMIT)
        up_pre = jnp.clip(jnp.dot(rows, w_up, preferred_element_type=jnp.float32), -CLAMP_LIMIT, CLAMP_LIMIT)
        hidden = ((up_pre + 1.0) * gate_pre * jax.nn.sigmoid(GLU_ALPHA * gate_pre)).astype(jnp.bfloat16)
        answer = jnp.dot(hidden, w_down, preferred_element_type=jnp.float32).astype(jnp.bfloat16)
        weight = mixing[picked]
        total = total.at[token_rows].add(answer.astype(jnp.float32) * weight[:, None])
        return (total, None)
    total, unused = lax.scan(one_expert, jnp.zeros((TOKENS + 1, D), jnp.float32), jnp.arange(EXPERTS, dtype=jnp.int32))
    mixed = total[:TOKENS].astype(jnp.bfloat16)
    return (gate_weights, up_weights, down_weights, mixed)
```

```python
import jax
import jax.numpy as jnp
from jax import lax
from jax.sharding import PartitionSpec as P

NORM_EPS = 1e-05
CLAMP_LIMIT = 7.0
GLU_ALPHA = 1.702


def normalize(tokens):
    values = tokens.astype(jnp.float32)
    centre = jnp.mean(values, -1, keepdims=True)
    spread = jnp.mean(jnp.square(values - centre), -1, keepdims=True)
    return ((values - centre) * lax.rsqrt(spread + NORM_EPS)).astype(jnp.bfloat16)


def dense_mixing(routes, route_scores, experts):
    mixing = jax.nn.softmax(route_scores, axis=-1)
    named = routes[:, :, None] == jnp.arange(experts, dtype=jnp.int32)[None, None, :]
    return jnp.sum(jnp.where(named, mixing[:, :, None], 0.0), axis=1)


def per_device(tokens, routes, route_scores, norm_gain, gate_master, up_master, down_master):
    experts = gate_master.shape[0]
    tok_count = tokens.shape[0]
    half = tok_count // lax.axis_size("tp")
    own_half = lax.dynamic_slice_in_dim(tokens, lax.axis_index("tp") * half, half, 0)
    rows = lax.all_gather(normalize(own_half), ("fs", "tp"), axis=0, tiled=True)
    share = dense_mixing(routes, route_scores, experts).T
    weight = lax.all_to_all(share, "fs", split_axis=0, concat_axis=0, tiled=True).reshape(-1, 1)

    def hand_over(low):
        moved = lax.all_to_all(low, "fs", split_axis=0, concat_axis=0, tiled=True)
        moved = lax.all_gather(moved, "gr", axis=0, tiled=True)
        return moved.reshape(1, moved.shape[0] * moved.shape[1], moved.shape[2])

    gate_weights = hand_over((norm_gain[None, :, None] * gate_master).astype(jnp.bfloat16))
    up_weights = hand_over((norm_gain[None, :, None] * up_master).astype(jnp.bfloat16))
    down_weights = hand_over(down_master.astype(jnp.bfloat16))
    gate_pre = jnp.minimum(
        jnp.dot(rows, gate_weights[0], preferred_element_type=jnp.float32), CLAMP_LIMIT
    )
    up_pre = jnp.clip(
        jnp.dot(rows, up_weights[0], preferred_element_type=jnp.float32), -CLAMP_LIMIT, CLAMP_LIMIT
    )
    hidden = ((up_pre + 1.0) * gate_pre * jax.nn.sigmoid(GLU_ALPHA * gate_pre)).astype(jnp.bfloat16)
    whole = lax.all_gather(hidden, "tp", axis=1, tiled=True)
    answer = jnp.dot(whole, down_weights[0], preferred_element_type=jnp.float32)
    part = (answer * weight).astype(jnp.bfloat16)
    mixed = lax.psum_scatter(part, "fs", scatter_dimension=0, tiled=True)
    return (gate_weights, up_weights, down_weights, mixed)


def solution(mesh):
    in_specs = (
        P(("gr", "fs"), None),
        P(("gr", "fs"), None),
        P(("gr", "fs"), None),
        P(("gr", "fs")),
        P(None, ("gr", "fs"), "tp"),
        P(None, ("gr", "fs"), "tp"),
        P(None, ("gr", "fs"), "tp"),
    )
    out_specs = (
        P("fs", None, "tp"),
        P("fs", None, "tp"),
        P("fs", None, "tp"),
        P(("gr", "fs"), "tp"),
    )
    return jax.shard_map(
        per_device, mesh=mesh, in_specs=in_specs, out_specs=out_specs, check_vma=False
    )
```

```python
import functools

import jax
import jax.numpy as jnp
from jax import lax
from jax.experimental import pallas as pl
from jax.experimental.pallas import tpu as pltpu
from jax.sharding import PartitionSpec as P

NORM_EPS = 1e-05
CLAMP_LIMIT = 7.0
GLU_ALPHA = 1.702
MESH = pl.DeviceIdType.MESH
COLUMN_TILE = 256
VMEM_LIMIT = 56 * 1024 * 1024


def normalize(tokens):
    values = tokens.astype(jnp.float32)
    centre = jnp.mean(values, -1, keepdims=True)
    spread = jnp.mean(jnp.square(values - centre), -1, keepdims=True)
    return ((values - centre) * lax.rsqrt(spread + NORM_EPS)).astype(jnp.bfloat16)


def dense_mixing(routes, route_scores, experts):
    mixing = jax.nn.softmax(route_scores, axis=-1)
    named = routes[:, :, None] == jnp.arange(experts, dtype=jnp.int32)[None, None, :]
    return jnp.sum(jnp.where(named, mixing[:, :, None], 0.0), axis=1)


def by_collectives(tokens, routes, route_scores, norm_gain, gate_master, up_master, down_master):
    experts = gate_master.shape[0]
    tok_count = tokens.shape[0]
    half = tok_count // lax.axis_size("tp")
    own_half = lax.dynamic_slice_in_dim(tokens, lax.axis_index("tp") * half, half, 0)
    rows = lax.all_gather(normalize(own_half), ("fs", "tp"), axis=0, tiled=True)
    share = dense_mixing(routes, route_scores, experts).T
    weight = lax.all_to_all(share, "fs", split_axis=0, concat_axis=0, tiled=True).reshape(-1, 1)

    def hand_over(low):
        moved = lax.all_to_all(low, "fs", split_axis=0, concat_axis=0, tiled=True)
        moved = lax.all_gather(moved, "gr", axis=0, tiled=True)
        return moved.reshape(1, moved.shape[0] * moved.shape[1], moved.shape[2])

    gate_weights = hand_over((norm_gain[None, :, None] * gate_master).astype(jnp.bfloat16))
    up_weights = hand_over((norm_gain[None, :, None] * up_master).astype(jnp.bfloat16))
    down_weights = hand_over(down_master.astype(jnp.bfloat16))
    gate_pre = jnp.minimum(
        jnp.dot(rows, gate_weights[0], preferred_element_type=jnp.float32), CLAMP_LIMIT
    )
    up_pre = jnp.clip(
        jnp.dot(rows, up_weights[0], preferred_element_type=jnp.float32), -CLAMP_LIMIT, CLAMP_LIMIT
    )
    hidden = ((up_pre + 1.0) * gate_pre * jax.nn.sigmoid(GLU_ALPHA * gate_pre)).astype(jnp.bfloat16)
    whole = lax.all_gather(hidden, "tp", axis=1, tiled=True)
    answer = jnp.dot(whole, down_weights[0], preferred_element_type=jnp.float32)
    part = (answer * weight).astype(jnp.bfloat16)
    mixed = lax.psum_scatter(part, "fs", scatter_dimension=0, tiled=True)
    return (gate_weights, up_weights, down_weights, mixed)


def greet(partners):
    barrier = pltpu.get_barrier_semaphore()
    for partner in partners:
        pl.semaphore_signal(barrier, inc=1, device_id=partner, device_id_type=MESH)
    pl.semaphore_wait(barrier, len(partners))


def hand_over_kernel(
    n_fs, gate, up, down, share, own, gate_out, up_out, down_out, share_out, rows_out,
    kept, kept_down, kept_share, kept_rows, keep_sem,
    out_send, out_recv, relay_send, relay_recv, share_send, share_recv,
    line_send, line_recv, cross_send, cross_recv, twin_send, twin_recv,
):
    gr, fs, tp = lax.axis_index("gr"), lax.axis_index("fs"), lax.axis_index("tp")
    n_z = n_fs // 2
    z, y = fs // 2, fs % 2
    lows, outs = (gate, up, down), (gate_out, up_out, down_out)

    def away(dz, dy):
        return lax.rem(z + dz, n_z) * 2 + lax.rem(y + dy, 2)

    greet(
        [{"fs": away(k // 2, k % 2)} for k in range(1, n_fs)]
        + [{"gr": 1 - gr}, {"tp": 1 - tp}]
    )

    stays_in = [
        pltpu.make_async_copy(gate.at[fs], kept.at[0], keep_sem.at[0]),
        pltpu.make_async_copy(up.at[fs], kept.at[1], keep_sem.at[1]),
        pltpu.make_async_copy(down.at[fs], kept_down, keep_sem.at[2]),
        pltpu.make_async_copy(share.at[fs], kept_share, keep_sem.at[3]),
        pltpu.make_async_copy(own, kept_rows, keep_sem.at[4]),
    ]
    stays_out = [
        pltpu.make_async_copy(kept.at[0], gate_out.at[gr * n_fs + fs], keep_sem.at[5]),
        pltpu.make_async_copy(kept.at[1], up_out.at[gr * n_fs + fs], keep_sem.at[6]),
        pltpu.make_async_copy(kept_down, down_out.at[gr * n_fs + fs], keep_sem.at[7]),
        pltpu.make_async_copy(kept_share, share_out.at[fs], keep_sem.at[8]),
        pltpu.make_async_copy(kept_rows, rows_out.at[fs, tp], keep_sem.at[9]),
    ]

    def copy(src, dst, send, recv, partner):
        return pltpu.make_async_remote_copy(
            src_ref=src, dst_ref=dst, send_sem=send, recv_sem=recv,
            device_id=partner, device_id_type=MESH,
        )

    def weight_copy(m, source, target):
        return copy(
            lows[m].at[target], outs[m].at[gr * n_fs + source],
            out_send.at[m, target], out_recv.at[m, source], {"fs": target},
        )

    def relay_copy(m, source, row_of, own_input):
        slot = outs[m].at[row_of * n_fs + source]
        src = lows[m].at[source] if own_input else slot
        return copy(src, slot, relay_send.at[m, source], relay_recv.at[m, source], {"gr": 1 - gr})

    def share_copy(source, target):
        return copy(
            share.at[target], share_out.at[source],
            share_send.at[target], share_recv.at[source], {"fs": target},
        )

    def block(zb, yb, from_own):
        return own if from_own else rows_out.at[zb * 2 + yb, tp]

    def line_copy(zb, toward, from_own):
        way = (toward + 1) // 2
        return copy(
            block(zb, y, from_own), rows_out.at[zb * 2 + y, tp],
            line_send.at[way, zb], line_recv.at[zb], {"fs": (z + toward) * 2 + y},
        )

    def cross_copy(zb, yb, from_own):
        return copy(
            block(zb, yb, from_own), rows_out.at[zb * 2 + yb, tp],
            cross_send.at[zb], cross_recv.at[zb], {"fs": z * 2 + 1 - y},
        )

    def twin_copy(zb, yb, core, from_own):
        slot = rows_out.at[zb * 2 + yb, core]
        src = own if from_own else slot
        return copy(
            src, slot, twin_send.at[zb * 2 + yb], twin_recv.at[zb * 2 + yb], {"tp": 1 - tp}
        )

    def send_weights(dz):
        for dy in range(2):
            if dz or dy:
                target = away(dz, dy)
                for m in range(3):
                    weight_copy(m, fs, target).start()

    def relay(dz):
        for dy in range(2):
            if dz or dy:
                source = away(n_z - dz, dy)
                for m in range(3):
                    weight_copy(m, source, fs).wait_recv()
                    relay_copy(m, source, gr, False).start()

    for held in stays_in:
        held.start()

    @pl.when(z > 0)
    def _():
        line_copy(z, -1, True).start()

    @pl.when(z < n_z - 1)
    def _():
        line_copy(z, 1, True).start()

    cross_copy(z, y, True).start()
    twin_copy(z, y, tp, True).start()
    for k in range(1, n_fs):
        share_copy(fs, away(k // 2, k % 2)).start()
    for m in range(3):
        copy(
            lows[m].at[fs], outs[m].at[gr * n_fs + fs],
            relay_send.at[m, fs], relay_recv.at[m, fs], {"gr": 1 - gr},
        ).start()
    send_weights(0)
    order = [d for k in range(1, n_z // 2 + 1) for d in dict.fromkeys((k, n_z - k))]
    for held, put in zip(stays_in, stays_out):
        held.wait()
        put.start()

    for k in range(1, n_z):
        send_weights(order[k - 1])

        @pl.when(z - k >= 0)
        def _():
            line_copy(z - k, 1, False).wait_recv()

            @pl.when(z < n_z - 1)
            def _():
                line_copy(z - k, 1, False).start()

            cross_copy(z - k, y, False).start()
            twin_copy(z - k, y, tp, False).start()

        @pl.when(z + k < n_z)
        def _():
            line_copy(z + k, -1, False).wait_recv()

            @pl.when(z > 0)
            def _():
                line_copy(z + k, -1, False).start()

            cross_copy(z + k, y, False).start()
            twin_copy(z + k, y, tp, False).start()

        relay(0 if k == 1 else order[k - 2])

    def crossed(zb):
        cross_copy(zb, 1 - y, False).wait_recv()
        twin_copy(zb, 1 - y, tp, False).start()

    for zb in range(n_z):
        crossed(zb)
    relay(order[n_z - 2])

    for zb in range(n_z):
        @pl.when(z > 0)
        def _():
            @pl.when(zb >= z)
            def _():
                line_copy(zb, -1, False).wait_send()

        @pl.when(z < n_z - 1)
        def _():
            @pl.when(zb <= z)
            def _():
                line_copy(zb, 1, False).wait_send()

        cross_copy(zb, y, False).wait_send()
    for k in range(n_fs):
        twin_copy(k // 2, k % 2, tp, False).wait_send()
        twin_copy(k // 2, k % 2, 1 - tp, False).wait_recv()
    for k in range(1, n_fs):
        other = away(k // 2, k % 2)
        share_copy(fs, other).wait_send()
        share_copy(other, fs).wait_recv()
        for m in range(3):
            weight_copy(m, fs, other).wait_send()
    for k in range(n_fs):
        for m in range(3):
            relay_copy(m, k, gr, False).wait_send()
            relay_copy(m, k, 1 - gr, False).wait_recv()
    for put in stays_out:
        put.wait()


def hand_over(gate_low, up_low, down_low, share, own):
    n_fs, n_gr, n_tp = (lax.axis_size(axis) for axis in ("fs", "gr", "tp"))
    half, width = own.shape
    like = jax.ShapeDtypeStruct
    dma = pltpu.SemaphoreType.DMA
    outs = [like((n_gr * n_fs,) + low.shape[1:], low.dtype) for low in (gate_low, up_low, down_low)]
    outs += [like(share.shape, share.dtype), like((n_fs, n_tp, half, width), own.dtype)]
    return pl.pallas_call(
        functools.partial(hand_over_kernel, n_fs),
        out_shape=outs,
        in_specs=[pl.BlockSpec(memory_space=pl.ANY)] * 5,
        out_specs=[pl.BlockSpec(memory_space=pl.ANY)] * 5,
        scratch_shapes=[
            pltpu.VMEM((2,) + gate_low.shape[1:], gate_low.dtype),
            pltpu.VMEM(down_low.shape[1:], down_low.dtype),
            pltpu.VMEM(share.shape[1:], share.dtype),
            pltpu.VMEM(own.shape, own.dtype),
            dma((10,)),
            dma((3, n_fs)), dma((3, n_fs)), dma((3, n_fs)), dma((3, n_fs)),
            dma((n_fs,)), dma((n_fs,)),
            dma((2, n_fs // 2)), dma((n_fs // 2,)),
            dma((n_fs // 2,)), dma((n_fs // 2,)),
            dma((n_fs,)), dma((n_fs,)),
        ],
        compiler_params=pltpu.CompilerParams(
            collective_id=0, has_side_effects=True, vmem_limit_bytes=VMEM_LIMIT
        ),
    )(gate_low, up_low, down_low, share, own)


def experts_kernel(
    n_fs, rows, gate, up, down, weight, out,
    hid_own, hid_got, ysend, ygot, zsend, zgot,
    hid_send, hid_recv, y_send, y_recv, z_send, z_recv,
):
    fs, tp = lax.axis_index("fs"), lax.axis_index("tp")
    n_z = n_fs // 2
    z, y = fs // 2, fs % 2
    hid_cols, out_cols = gate.shape[1], down.shape[1]
    greet(
        [{"fs": lax.rem(z + k, n_z) * 2 + y} for k in range(1, n_z)]
        + [{"fs": z * 2 + 1 - y}, {"tp": 1 - tp}]
    )

    def copy(src, dst, send, recv, partner):
        return pltpu.make_async_remote_copy(
            src_ref=src, dst_ref=dst, send_sem=send, recv_sem=recv,
            device_id=partner, device_id_type=MESH,
        )

    def hid_copy(j):
        return copy(
            hid_own.at[j], hid_got.at[j], hid_send.at[j], hid_recv.at[j], {"tp": 1 - tp}
        )

    def y_copy(i):
        return copy(ysend.at[i], ygot.at[i], y_send.at[i], y_recv.at[i], {"fs": z * 2 + 1 - y})

    def z_copy(i):
        target = lax.rem(z + n_z - 1 - i, n_z) * 2 + y
        return copy(zsend.at[i], zgot.at[i], z_send.at[i], z_recv.at[i], {"fs": target})

    def target_of(j):
        phase, i = j // n_z, j % n_z
        return lax.rem(z + n_z - 1 - i, n_z) * 2 + lax.rem(y + 1 + phase, 2)

    def fill_hidden(j):
        block = target_of(j)

        @pl.loop(0, hid_cols // COLUMN_TILE)
        def _(c):
            cols = pl.ds(pl.multiple_of(c * COLUMN_TILE, COLUMN_TILE), COLUMN_TILE)
            gate_pre = jnp.minimum(
                jnp.dot(rows[block], gate[:, cols], preferred_element_type=jnp.float32),
                CLAMP_LIMIT,
            )
            up_pre = jnp.clip(
                jnp.dot(rows[block], up[:, cols], preferred_element_type=jnp.float32),
                -CLAMP_LIMIT,
                CLAMP_LIMIT,
            )
            hidden = (up_pre + 1.0) * gate_pre * jax.nn.sigmoid(GLU_ALPHA * gate_pre)
            hid_own[j, :, cols] = hidden.astype(jnp.bfloat16)

        hid_copy(j).start()

    def weighted(j, cols):
        mine = pl.ds(pl.multiple_of(tp * hid_cols, hid_cols), hid_cols)
        theirs = pl.ds(pl.multiple_of((1 - tp) * hid_cols, hid_cols), hid_cols)
        answer = jnp.dot(hid_own[j], down[mine, cols], preferred_element_type=jnp.float32)
        answer += jnp.dot(hid_got[j], down[theirs, cols], preferred_element_type=jnp.float32)
        return answer * weight[target_of(j)]

    def tiles(body):
        @pl.loop(0, out_cols // COLUMN_TILE)
        def _(c):
            body(pl.ds(pl.multiple_of(c * COLUMN_TILE, COLUMN_TILE), COLUMN_TILE))

    fill_hidden(0)

    @pl.loop(0, n_fs)
    def _(p):
        @pl.when(p < n_fs - 1)
        def _():
            fill_hidden(p + 1)

        hid_copy(p).wait_recv()

        @pl.when(p < n_z)
        def _():
            def body(cols):
                ysend[p, :, cols] = weighted(p, cols).astype(jnp.bfloat16)

            tiles(body)
            y_copy(p).start()

        @pl.when(p >= n_z)
        def _():
            i = p - n_z
            y_copy(i).wait_recv()

            def body(cols):
                total = weighted(p, cols) + ygot[i, :, cols].astype(jnp.float32)
                zsend[i, :, cols] = total.astype(jnp.bfloat16)

            tiles(body)

            @pl.when(i < n_z - 1)
            def _():
                z_copy(i).start()

    for i in range(n_z - 1):
        z_copy(i).wait_recv()

    def close(cols):
        total = zsend[n_z - 1, :, cols].astype(jnp.float32)
        for i in range(n_z - 1):
            total += zgot[i, :, cols].astype(jnp.float32)
        out[:, cols] = total.astype(jnp.bfloat16)

    tiles(close)
    for j in range(n_fs):
        hid_copy(j).wait_send()
    for i in range(n_z):
        y_copy(i).wait_send()
    for i in range(n_z - 1):
        z_copy(i).wait_send()


def experts_here(rows, gate, up, down, weight):
    n_fs, tok_count, width = rows.shape
    n_z = n_fs // 2
    hid_cols, out_cols = gate.shape[1], down.shape[1]
    dma = pltpu.SemaphoreType.DMA
    low = jnp.bfloat16
    return pl.pallas_call(
        functools.partial(experts_kernel, n_fs),
        out_shape=jax.ShapeDtypeStruct((tok_count, out_cols), low),
        in_specs=[pl.BlockSpec(memory_space=pltpu.VMEM)] * 5,
        out_specs=pl.BlockSpec(memory_space=pltpu.VMEM),
        scratch_shapes=[
            pltpu.VMEM((n_fs, tok_count, hid_cols), low),
            pltpu.VMEM((n_fs, tok_count, hid_cols), low),
            pltpu.VMEM((n_z, tok_count, out_cols), low),
            pltpu.VMEM((n_z, tok_count, out_cols), low),
            pltpu.VMEM((n_z, tok_count, out_cols), low),
            pltpu.VMEM((n_z - 1, tok_count, out_cols), low),
            dma((n_fs,)), dma((n_fs,)),
            dma((n_z,)), dma((n_z,)),
            dma((n_z - 1,)), dma((n_z - 1,)),
        ],
        compiler_params=pltpu.CompilerParams(
            collective_id=1, has_side_effects=True, vmem_limit_bytes=VMEM_LIMIT
        ),
    )(rows, gate, up, down, weight)


def fits_in_kernels(tokens, gate_master):
    n_fs, n_gr, n_tp = (lax.axis_size(axis) for axis in ("fs", "gr", "tp"))
    tok_count, width = tokens.shape
    held = 2 * n_fs * tok_count * (width + 5 * gate_master.shape[2])
    return n_fs % 2 == 0 and n_gr == 2 and n_tp == 2 and held < VMEM_LIMIT * 3 // 4


def per_device(tokens, routes, route_scores, norm_gain, gate_master, up_master, down_master):
    if not fits_in_kernels(tokens, gate_master):
        return by_collectives(
            tokens, routes, route_scores, norm_gain, gate_master, up_master, down_master
        )
    experts, n_fs = gate_master.shape[0], lax.axis_size("fs")
    tok_count, width = tokens.shape
    half = tok_count // lax.axis_size("tp")
    own = normalize(lax.dynamic_slice_in_dim(tokens, lax.axis_index("tp") * half, half, 0))
    share = dense_mixing(routes, route_scores, experts).T.reshape(experts, 1, tok_count)
    gate, up, down, weight, rows = hand_over(
        (norm_gain[None, :, None] * gate_master).astype(jnp.bfloat16),
        (norm_gain[None, :, None] * up_master).astype(jnp.bfloat16),
        down_master.astype(jnp.bfloat16),
        share,
        own,
    )
    gate = gate.reshape(-1, gate.shape[2])
    up = up.reshape(-1, up.shape[2])
    down = down.reshape(-1, down.shape[2])
    mixed = experts_here(
        rows.reshape(n_fs, tok_count, width), gate, up, down, weight.reshape(n_fs, tok_count, 1)
    )
    return (gate[None], up[None], down[None], mixed)


def solution(mesh):
    in_specs = (
        P(("gr", "fs"), None),
        P(("gr", "fs"), None),
        P(("gr", "fs"), None),
        P(("gr", "fs")),
        P(None, ("gr", "fs"), "tp"),
        P(None, ("gr", "fs"), "tp"),
        P(None, ("gr", "fs"), "tp"),
    )
    out_specs = (
        P("fs", None, "tp"),
        P("fs", None, "tp"),
        P("fs", None, "tp"),
        P(("gr", "fs"), "tp"),
    )
    return jax.shard_map(
        per_device, mesh=mesh, in_specs=in_specs, out_specs=out_specs, check_vma=False
    )
```

```python
import functools

import jax
import jax.numpy as jnp
from jax import lax
from jax.experimental import pallas as pl
from jax.experimental.pallas import tpu as pltpu
from jax.sharding import PartitionSpec as P

NORM_EPS = 1e-05
CLAMP_LIMIT = 7.0
GLU_ALPHA = 1.702
MESH = pl.DeviceIdType.MESH
COLUMN_TILE = 256
VMEM_LIMIT = 56 * 1024 * 1024


def normalize(tokens):
    values = tokens.astype(jnp.float32)
    centre = jnp.mean(values, -1, keepdims=True)
    spread = jnp.mean(jnp.square(values - centre), -1, keepdims=True)
    return ((values - centre) * lax.rsqrt(spread + NORM_EPS)).astype(jnp.bfloat16)


def dense_mixing(routes, route_scores, experts):
    mixing = jax.nn.softmax(route_scores, axis=-1)
    named = routes[:, :, None] == jnp.arange(experts, dtype=jnp.int32)[None, None, :]
    return jnp.sum(jnp.where(named, mixing[:, :, None], 0.0), axis=1)


def by_collectives(tokens, routes, route_scores, norm_gain, gate_master, up_master, down_master):
    experts = gate_master.shape[0]
    tok_count = tokens.shape[0]
    half = tok_count // lax.axis_size("tp")
    own_half = lax.dynamic_slice_in_dim(tokens, lax.axis_index("tp") * half, half, 0)
    rows = lax.all_gather(normalize(own_half), ("fs", "tp"), axis=0, tiled=True)
    share = dense_mixing(routes, route_scores, experts).T
    weight = lax.all_to_all(share, "fs", split_axis=0, concat_axis=0, tiled=True).reshape(-1, 1)

    def hand_over(low):
        moved = lax.all_to_all(low, "fs", split_axis=0, concat_axis=0, tiled=True)
        moved = lax.all_gather(moved, "gr", axis=0, tiled=True)
        return moved.reshape(1, moved.shape[0] * moved.shape[1], moved.shape[2])

    gate_weights = hand_over((norm_gain[None, :, None] * gate_master).astype(jnp.bfloat16))
    up_weights = hand_over((norm_gain[None, :, None] * up_master).astype(jnp.bfloat16))
    down_weights = hand_over(down_master.astype(jnp.bfloat16))
    gate_pre = jnp.minimum(
        jnp.dot(rows, gate_weights[0], preferred_element_type=jnp.float32), CLAMP_LIMIT
    )
    up_pre = jnp.clip(
        jnp.dot(rows, up_weights[0], preferred_element_type=jnp.float32), -CLAMP_LIMIT, CLAMP_LIMIT
    )
    hidden = ((up_pre + 1.0) * gate_pre * jax.nn.sigmoid(GLU_ALPHA * gate_pre)).astype(jnp.bfloat16)
    whole = lax.all_gather(hidden, "tp", axis=1, tiled=True)
    answer = jnp.dot(whole, down_weights[0], preferred_element_type=jnp.float32)
    part = (answer * weight).astype(jnp.bfloat16)
    mixed = lax.psum_scatter(part, "fs", scatter_dimension=0, tiled=True)
    return (gate_weights, up_weights, down_weights, mixed)


def greet(partners):
    barrier = pltpu.get_barrier_semaphore()
    for partner in partners:
        pl.semaphore_signal(barrier, inc=1, device_id=partner, device_id_type=MESH)
    pl.semaphore_wait(barrier, len(partners))


def hand_over_kernel(
    n_fs, gate, up, down, share, own, gate_out, up_out, down_out, share_out, rows_out,
    kept, kept_down, kept_share, kept_rows, keep_sem,
    out_send, out_recv, relay_send, relay_recv, share_send, share_recv,
    line_send, line_recv, cross_send, cross_recv, twin_send, twin_recv,
):
    gr, fs, tp = lax.axis_index("gr"), lax.axis_index("fs"), lax.axis_index("tp")
    n_z = n_fs // 2
    z, y = fs // 2, fs % 2
    lows, outs = (gate, up, down), (gate_out, up_out, down_out)

    def away(dz, dy):
        return lax.rem(z + dz, n_z) * 2 + lax.rem(y + dy, 2)

    greet(
        [{"fs": away(k // 2, k % 2)} for k in range(1, n_fs)]
        + [{"gr": 1 - gr}, {"tp": 1 - tp}]
    )

    stays_in = [
        pltpu.make_async_copy(gate.at[fs], kept.at[0], keep_sem.at[0]),
        pltpu.make_async_copy(up.at[fs], kept.at[1], keep_sem.at[1]),
        pltpu.make_async_copy(down.at[fs], kept_down, keep_sem.at[2]),
        pltpu.make_async_copy(share.at[fs], kept_share, keep_sem.at[3]),
        pltpu.make_async_copy(own, kept_rows, keep_sem.at[4]),
    ]
    stays_out = [
        pltpu.make_async_copy(kept.at[0], gate_out.at[gr * n_fs + fs], keep_sem.at[5]),
        pltpu.make_async_copy(kept.at[1], up_out.at[gr * n_fs + fs], keep_sem.at[6]),
        pltpu.make_async_copy(kept_down, down_out.at[gr * n_fs + fs], keep_sem.at[7]),
        pltpu.make_async_copy(kept_share, share_out.at[fs], keep_sem.at[8]),
        pltpu.make_async_copy(kept_rows, rows_out.at[fs, tp], keep_sem.at[9]),
    ]

    def copy(src, dst, send, recv, partner):
        return pltpu.make_async_remote_copy(
            src_ref=src, dst_ref=dst, send_sem=send, recv_sem=recv,
            device_id=partner, device_id_type=MESH,
        )

    def weight_copy(m, source, target):
        return copy(
            lows[m].at[target], outs[m].at[gr * n_fs + source],
            out_send.at[m, target], out_recv.at[m, source], {"fs": target},
        )

    def relay_copy(m, source, row_of, own_input):
        slot = outs[m].at[row_of * n_fs + source]
        src = lows[m].at[source] if own_input else slot
        return copy(src, slot, relay_send.at[m, source], relay_recv.at[m, source], {"gr": 1 - gr})

    def share_copy(source, target):
        return copy(
            share.at[target], share_out.at[source],
            share_send.at[target], share_recv.at[source], {"fs": target},
        )

    def block(zb, yb, from_own):
        return own if from_own else rows_out.at[zb * 2 + yb, tp]

    def line_copy(zb, toward, from_own):
        way = (toward + 1) // 2
        return copy(
            block(zb, y, from_own), rows_out.at[zb * 2 + y, tp],
            line_send.at[way, zb], line_recv.at[zb], {"fs": (z + toward) * 2 + y},
        )

    def cross_copy(zb, yb, from_own):
        return copy(
            block(zb, yb, from_own), rows_out.at[zb * 2 + yb, tp],
            cross_send.at[zb], cross_recv.at[zb], {"fs": z * 2 + 1 - y},
        )

    def twin_copy(zb, yb, core, from_own):
        slot = rows_out.at[zb * 2 + yb, core]
        src = own if from_own else slot
        return copy(
            src, slot, twin_send.at[zb * 2 + yb], twin_recv.at[zb * 2 + yb], {"tp": 1 - tp}
        )

    def send_weights(dz):
        for dy in range(2):
            if dz or dy:
                target = away(dz, dy)
                for m in range(3):
                    weight_copy(m, fs, target).start()

    def relay(dz):
        for dy in range(2):
            if dz or dy:
                source = away(n_z - dz, dy)
                for m in range(3):
                    weight_copy(m, source, fs).wait_recv()
                    relay_copy(m, source, gr, False).start()

    for held in stays_in:
        held.start()

    @pl.when(z > 0)
    def _():
        line_copy(z, -1, True).start()

    @pl.when(z < n_z - 1)
    def _():
        line_copy(z, 1, True).start()

    cross_copy(z, y, True).start()
    twin_copy(z, y, tp, True).start()
    for k in range(1, n_fs):
        share_copy(fs, away(k // 2, k % 2)).start()
    for m in range(3):
        copy(
            lows[m].at[fs], outs[m].at[gr * n_fs + fs],
            relay_send.at[m, fs], relay_recv.at[m, fs], {"gr": 1 - gr},
        ).start()
    send_weights(0)
    order = [d for k in range(1, n_z // 2 + 1) for d in dict.fromkeys((k, n_z - k))]
    for held, put in zip(stays_in, stays_out):
        held.wait()
        put.start()

    for k in range(1, n_z):
        send_weights(order[k - 1])

        @pl.when(z - k >= 0)
        def _():
            line_copy(z - k, 1, False).wait_recv()

            @pl.when(z < n_z - 1)
            def _():
                line_copy(z - k, 1, False).start()

            cross_copy(z - k, y, False).start()
            twin_copy(z - k, y, tp, False).start()

        @pl.when(z + k < n_z)
        def _():
            line_copy(z + k, -1, False).wait_recv()

            @pl.when(z > 0)
            def _():
                line_copy(z + k, -1, False).start()

            cross_copy(z + k, y, False).start()
            twin_copy(z + k, y, tp, False).start()

        relay(0 if k == 1 else order[k - 2])

    def crossed(zb):
        cross_copy(zb, 1 - y, False).wait_recv()
        twin_copy(zb, 1 - y, tp, False).start()

    relay(order[n_z - 2])
    for zb in range(n_z):
        crossed(zb)

    for zb in range(n_z):
        @pl.when(z > 0)
        def _():
            @pl.when(zb >= z)
            def _():
                line_copy(zb, -1, False).wait_send()

        @pl.when(z < n_z - 1)
        def _():
            @pl.when(zb <= z)
            def _():
                line_copy(zb, 1, False).wait_send()

        cross_copy(zb, y, False).wait_send()
    for k in range(n_fs):
        twin_copy(k // 2, k % 2, tp, False).wait_send()
        twin_copy(k // 2, k % 2, 1 - tp, False).wait_recv()
    for k in range(1, n_fs):
        other = away(k // 2, k % 2)
        share_copy(fs, other).wait_send()
        share_copy(other, fs).wait_recv()
        for m in range(3):
            weight_copy(m, fs, other).wait_send()
    for k in range(n_fs):
        for m in range(3):
            relay_copy(m, k, gr, False).wait_send()
            relay_copy(m, k, 1 - gr, False).wait_recv()
    for put in stays_out:
        put.wait()


def hand_over(gate_low, up_low, down_low, share, own):
    n_fs, n_gr, n_tp = (lax.axis_size(axis) for axis in ("fs", "gr", "tp"))
    half, width = own.shape
    like = jax.ShapeDtypeStruct
    dma = pltpu.SemaphoreType.DMA
    outs = [like((n_gr * n_fs,) + low.shape[1:], low.dtype) for low in (gate_low, up_low, down_low)]
    outs += [like(share.shape, share.dtype), like((n_fs, n_tp, half, width), own.dtype)]
    return pl.pallas_call(
        functools.partial(hand_over_kernel, n_fs),
        out_shape=outs,
        in_specs=[pl.BlockSpec(memory_space=pl.ANY)] * 5,
        out_specs=[pl.BlockSpec(memory_space=pl.ANY)] * 5,
        scratch_shapes=[
            pltpu.VMEM((2,) + gate_low.shape[1:], gate_low.dtype),
            pltpu.VMEM(down_low.shape[1:], down_low.dtype),
            pltpu.VMEM(share.shape[1:], share.dtype),
            pltpu.VMEM(own.shape, own.dtype),
            dma((10,)),
            dma((3, n_fs)), dma((3, n_fs)), dma((3, n_fs)), dma((3, n_fs)),
            dma((n_fs,)), dma((n_fs,)),
            dma((2, n_fs // 2)), dma((n_fs // 2,)),
            dma((n_fs // 2,)), dma((n_fs // 2,)),
            dma((n_fs,)), dma((n_fs,)),
        ],
        compiler_params=pltpu.CompilerParams(
            collective_id=0, has_side_effects=True, vmem_limit_bytes=VMEM_LIMIT
        ),
    )(gate_low, up_low, down_low, share, own)


def experts_kernel(
    n_fs, rows, gate, up, down, weight, out,
    hid_own, hid_got, ysend, ygot, zsend, zgot,
    hid_send, hid_recv, y_send, y_recv, z_send, z_recv,
):
    fs, tp = lax.axis_index("fs"), lax.axis_index("tp")
    n_z = n_fs // 2
    z, y = fs // 2, fs % 2
    hid_cols, out_cols = gate.shape[1], down.shape[1]
    greet(
        [{"fs": lax.rem(z + k, n_z) * 2 + y} for k in range(1, n_z)]
        + [{"fs": z * 2 + 1 - y}, {"tp": 1 - tp}]
    )

    def copy(src, dst, send, recv, partner):
        return pltpu.make_async_remote_copy(
            src_ref=src, dst_ref=dst, send_sem=send, recv_sem=recv,
            device_id=partner, device_id_type=MESH,
        )

    def hid_copy(j):
        return copy(
            hid_own.at[j], hid_got.at[j], hid_send.at[j], hid_recv.at[j], {"tp": 1 - tp}
        )

    def y_copy(i, c):
        return copy(
            ysend.at[i, c], ygot.at[i, c], y_send.at[i, c], y_recv.at[i, c],
            {"fs": z * 2 + 1 - y},
        )

    def z_copy(i, c):
        target = lax.rem(z + n_z - 1 - i, n_z) * 2 + y
        return copy(
            zsend.at[i, c], zgot.at[i, c], z_send.at[i, c], z_recv.at[i, c], {"fs": target}
        )

    def place(j):
        last = j // (n_fs - 1)
        phase = ((j + 1) % 2) * ((j + n_fs - 1) // n_fs) + last
        return phase, (1 - phase) * ((j + 1) // 2) + phase * (j // 2 - 1 + last)

    def target_of(j):
        phase, i = place(j)
        return lax.rem(z + n_z - 1 - i, n_z) * 2 + lax.rem(y + 1 + phase, 2)

    def fill_hidden(j):
        block = target_of(j)

        @pl.loop(0, hid_cols // COLUMN_TILE)
        def _(c):
            cols = pl.ds(pl.multiple_of(c * COLUMN_TILE, COLUMN_TILE), COLUMN_TILE)
            gate_pre = jnp.minimum(
                jnp.dot(rows[block], gate[:, cols], preferred_element_type=jnp.float32),
                CLAMP_LIMIT,
            )
            up_pre = jnp.clip(
                jnp.dot(rows[block], up[:, cols], preferred_element_type=jnp.float32),
                -CLAMP_LIMIT,
                CLAMP_LIMIT,
            )
            hidden = (up_pre + 1.0) * gate_pre * jax.nn.sigmoid(GLU_ALPHA * gate_pre)
            hid_own[j, :, cols] = hidden.astype(jnp.bfloat16)

        hid_copy(j).start()

    def weighted(j, cols):
        mine = pl.ds(pl.multiple_of(tp * hid_cols, hid_cols), hid_cols)
        theirs = pl.ds(pl.multiple_of((1 - tp) * hid_cols, hid_cols), hid_cols)
        answer = jnp.dot(hid_own[j], down[mine, cols], preferred_element_type=jnp.float32)
        answer += jnp.dot(hid_got[j], down[theirs, cols], preferred_element_type=jnp.float32)
        return answer * weight[target_of(j)]

    count = out_cols // COLUMN_TILE

    def tiles(body):
        @pl.loop(0, count)
        def _(c):
            body(c, pl.ds(pl.multiple_of(c * COLUMN_TILE, COLUMN_TILE), COLUMN_TILE))

    fill_hidden(0)

    @pl.loop(0, n_fs)
    def _(p):
        @pl.when(p < n_fs - 1)
        def _():
            fill_hidden(p + 1)

        hid_copy(p).wait_recv()

        phase, i = place(p)

        @pl.when(phase == 0)
        def _():
            def body(c, cols):
                ysend[i, c] = weighted(p, cols).astype(jnp.bfloat16)
                y_copy(i, c).start()

            tiles(body)

        @pl.when(phase == 1)
        def _():
            def body(c, cols):
                y_copy(i, c).wait_recv()
                total = weighted(p, cols) + ygot[i, c].astype(jnp.float32)
                zsend[i, c] = total.astype(jnp.bfloat16)

                @pl.when(i < n_z - 1)
                def _():
                    z_copy(i, c).start()

            tiles(body)

    def close(c, cols):
        total = zsend[n_z - 1, c].astype(jnp.float32)
        for i in range(n_z - 1):
            z_copy(i, c).wait_recv()
            total += zgot[i, c].astype(jnp.float32)
        out[:, cols] = total.astype(jnp.bfloat16)

    tiles(close)
    for j in range(n_fs):
        hid_copy(j).wait_send()

    @pl.loop(0, count)
    def _(c):
        for i in range(n_z):
            y_copy(i, c).wait_send()
        for i in range(n_z - 1):
            z_copy(i, c).wait_send()


def experts_here(rows, gate, up, down, weight):
    n_fs, tok_count, width = rows.shape
    n_z = n_fs // 2
    hid_cols, out_cols = gate.shape[1], down.shape[1]
    count = out_cols // COLUMN_TILE
    dma = pltpu.SemaphoreType.DMA
    low = jnp.bfloat16
    return pl.pallas_call(
        functools.partial(experts_kernel, n_fs),
        out_shape=jax.ShapeDtypeStruct((tok_count, out_cols), low),
        in_specs=[pl.BlockSpec(memory_space=pltpu.VMEM)] * 5,
        out_specs=pl.BlockSpec(memory_space=pltpu.VMEM),
        scratch_shapes=[
            pltpu.VMEM((n_fs, tok_count, hid_cols), low),
            pltpu.VMEM((n_fs, tok_count, hid_cols), low),
            pltpu.VMEM((n_z, count, tok_count, COLUMN_TILE), low),
            pltpu.VMEM((n_z, count, tok_count, COLUMN_TILE), low),
            pltpu.VMEM((n_z, count, tok_count, COLUMN_TILE), low),
            pltpu.VMEM((n_z - 1, count, tok_count, COLUMN_TILE), low),
            dma((n_fs,)), dma((n_fs,)),
            dma((n_z, count)), dma((n_z, count)),
            dma((n_z - 1, count)), dma((n_z - 1, count)),
        ],
        compiler_params=pltpu.CompilerParams(
            collective_id=1, has_side_effects=True, vmem_limit_bytes=VMEM_LIMIT
        ),
    )(rows, gate, up, down, weight)


def fits_in_kernels(tokens, gate_master):
    n_fs, n_gr, n_tp = (lax.axis_size(axis) for axis in ("fs", "gr", "tp"))
    tok_count, width = tokens.shape
    held = 2 * n_fs * tok_count * (width + 5 * gate_master.shape[2])
    return n_fs % 2 == 0 and n_gr == 2 and n_tp == 2 and held < VMEM_LIMIT * 3 // 4


def per_device(tokens, routes, route_scores, norm_gain, gate_master, up_master, down_master):
    if not fits_in_kernels(tokens, gate_master):
        return by_collectives(
            tokens, routes, route_scores, norm_gain, gate_master, up_master, down_master
        )
    experts, n_fs = gate_master.shape[0], lax.axis_size("fs")
    tok_count, width = tokens.shape
    half = tok_count // lax.axis_size("tp")
    own = normalize(lax.dynamic_slice_in_dim(tokens, lax.axis_index("tp") * half, half, 0))
    share = dense_mixing(routes, route_scores, experts).T.reshape(experts, 1, tok_count)
    gate, up, down, weight, rows = hand_over(
        (norm_gain[None, :, None] * gate_master).astype(jnp.bfloat16),
        (norm_gain[None, :, None] * up_master).astype(jnp.bfloat16),
        down_master.astype(jnp.bfloat16),
        share,
        own,
    )
    gate = gate.reshape(-1, gate.shape[2])
    up = up.reshape(-1, up.shape[2])
    down = down.reshape(-1, down.shape[2])
    mixed = experts_here(
        rows.reshape(n_fs, tok_count, width), gate, up, down, weight.reshape(n_fs, tok_count, 1)
    )
    return (gate[None], up[None], down[None], mixed)


def solution(mesh):
    in_specs = (
        P(("gr", "fs"), None),
        P(("gr", "fs"), None),
        P(("gr", "fs"), None),
        P(("gr", "fs")),
        P(None, ("gr", "fs"), "tp"),
        P(None, ("gr", "fs"), "tp"),
        P(None, ("gr", "fs"), "tp"),
    )
    out_specs = (
        P("fs", None, "tp"),
        P("fs", None, "tp"),
        P("fs", None, "tp"),
        P(("gr", "fs"), "tp"),
    )
    return jax.shard_map(
        per_device, mesh=mesh, in_specs=in_specs, out_specs=out_specs, check_vma=False
    )
```
